256 devices in a mesh: fs: 32 (over z, x), rep: 4 (over y), tp: 2 (over core).
Axes of the slice: x: 4, y: 4, z: 8, core: 2. Of those that a mesh axis runs over, the one named last changes fastest.
Arguments:
- saved_input: bfloat16 [131072, 2048], P(('fs', 'rep')), may hold values from -500 to 500
- query_cotangent: bfloat16 [131072, 2048], P(('fs', 'rep'), 'tp'), may hold values from -0.0049438477 to 0.0049438477
- key_cotangent: bfloat16 [131072, 512], P(('fs', 'rep'), 'tp'), may hold values from -0.0049438477 to 0.0049438477
- query_weight: float32 [2048, 2048], P('fs', 'tp'), may hold values from -45 to 45
- key_weight: float32 [2048, 512], P('fs', 'tp'), may hold values from -45 to 45
- query_moment: float32 [2048, 2048], P('fs', 'tp'), may hold values from -45 to 45
- key_moment: float32 [2048, 512], P('fs', 'tp'), may hold values from -45 to 45
- query_row_root: bfloat16 [2048, 2048], P('fs'), may hold values from -1 to 3, as said below
- key_row_root: bfloat16 [2048, 2048], P('fs'), may hold values from -1 to 3, as said below
- query_head_root: bfloat16 [32, 64, 64], P('tp'), may hold values from -1 to 3, as said below
- key_head_root: bfloat16 [8, 64, 64], P('tp'), may hold values from -1 to 3, as said below
- query_head_stat: float32 [32, 64, 64], P('tp'), may hold values from -26 to 27, as said below
- key_head_stat: float32 [8, 64, 64], P('tp'), may hold values from -26 to 27, as said below
Outputs:
- query_step: float32 [2048, 2048], P('fs', 'tp')
- key_step: float32 [2048, 512], P('fs', 'tp')
- query_next: float32 [2048, 2048], P('fs', 'tp')
- key_next: float32 [2048, 512], P('fs', 'tp')
- query_copy: bfloat16 [2048, 2048], P(None, 'tp')
- key_copy: bfloat16 [2048, 512], P(None, 'tp')
- query_moment_next: float32 [2048, 2048], P('fs', 'tp')
- key_moment_next: float32 [2048, 512], P('fs', 'tp')
- query_stat_next: float32 [32, 64, 64], P('tp')
- key_stat_next: float32 [8, 64, 64], P('tp')
The draws below stay inside these ranges and needn't reach their ends.
Inputs may be any that keep to these rules, and one draw needn't show every extreme that they name: `query_row_root`: symmetric. `key_row_root`: symmetric. `query_head_root`: each head's matrix is symmetric. `key_head_root`: each head's matrix is symmetric. `query_head_stat`: each head's matrix is symmetric. `key_head_stat`: each head's matrix is symmetric.
All inputs are finite; a program needn't handle non-finite values.
Results may differ from the reference program's by a relative error of at most 0.0018.
The reference program's roundings to bfloat16 on the way count: a program that leaves them out, or rounds other values in their place, can miss the bound.
Values may be sent and summed in bfloat16 or wider, within the bound.
No kernel may reach another device: no remote copies, remote signals or barrier semaphores. Data moves between devices by JAX's collectives and lax.ppermute only.
A program may use at most 128 MiB of HBM per device.

```python
import math
import jax
import jax.numpy as jnp
from jax import lax

D = 2048
HEAD_DIM = 64
QHEADS = 32
KVHEADS = 8
TOKENS = 131072
QW = 2048
KW = 512


def rising_scale(length):
    return jnp.exp(jnp.linspace(math.log(0.3), math.log(3.0), length)).astype(jnp.float32)


def column_rise(length):
    return jnp.exp(jnp.linspace(0.0, math.log(10.0), length)).astype(jnp.float32)


def bounded_entries(rng_key, shape):
    return jax.random.truncated_normal(rng_key, -5.0, 5.0, shape, jnp.float32)


def matrix_draw(key, marker, row_total, col_total):
    first_key, second_key = jax.random.split(jax.random.fold_in(key, marker))
    entries = bounded_entries(first_key, (row_total, col_total))
    col_scale = jnp.exp(jax.random.uniform(second_key, (1, col_total), jnp.float32, math.log(0.3), math.log(3.0)))
    return entries * rising_scale(row_total)[:, None] * col_scale


def root_draw(key, marker, count_mats, order):
    first_key, second_key = jax.random.split(jax.random.fold_in(key, marker))
    diagonal = jnp.exp(jax.random.uniform(first_key, (count_mats, order), jnp.float32, math.log(0.5), math.log(2.0)))
    off_diagonal = bounded_entries(second_key, (count_mats, order, order)) * (0.7 / math.sqrt(order))
    symmetric = 0.5 * (off_diagonal + jnp.swapaxes(off_diagonal, 1, 2))
    identity = jnp.eye(order, dtype=jnp.float32)[None]
    return symmetric * (1.0 - identity) + diagonal[:, :, None] * identity


def stat_draw(key, marker, count_mats):
    factor = bounded_entries(jax.random.fold_in(key, marker), (count_mats, HEAD_DIM, HEAD_DIM))
    gram = jnp.einsum('hde,hfe->hdf', factor, factor, precision=jax.lax.Precision.HIGHEST) / HEAD_DIM
    return gram + 0.6 * jnp.eye(HEAD_DIM, dtype=jnp.float32)[None]


def draw_saved_input(key, part):
    first_key, second_key = jax.random.split(jax.random.fold_in(key, 101))
    entries = bounded_entries(first_key, (TOKENS, D))
    token_scale = jnp.exp(jax.random.uniform(second_key, (TOKENS, 1), jnp.float32, 0.0, math.log(10.0)))
    return (entries * token_scale * column_rise(D)[None, :]).astype(jnp.bfloat16)


def draw_query_weight(key, part):
    return matrix_draw(key, 201, D, QHEADS * HEAD_DIM)


def draw_key_weight(key, part):
    return matrix_draw(key, 202, D, KVHEADS * HEAD_DIM)


def draw_query_moment(key, part):
    return matrix_draw(key, 203, D, QHEADS * HEAD_DIM)


def draw_key_moment(key, part):
    return matrix_draw(key, 204, D, KVHEADS * HEAD_DIM)


def draw_query_row_root(key, part):
    return root_draw(key, 301, 1, D)[0].astype(jnp.bfloat16)


def draw_key_row_root(key, part):
    return root_draw(key, 302, 1, D)[0].astype(jnp.bfloat16)


def draw_query_head_root(key, part):
    return root_draw(key, 303, QHEADS, HEAD_DIM).astype(jnp.bfloat16)


def draw_key_head_root(key, part):
    return root_draw(key, 304, KVHEADS, HEAD_DIM).astype(jnp.bfloat16)


def draw_query_head_stat(key, part):
    return stat_draw(key, 401, QHEADS)


def draw_key_head_stat(key, part):
    return stat_draw(key, 402, KVHEADS)


def block_levels(rng, extent, cuts, smallest, largest):
    loudness = 1.0
    for axis_at, parts in cuts:
        heights = jax.random.uniform(jax.random.fold_in(jax.random.fold_in(rng, 6), axis_at), (parts,), jnp.float32, smallest / len(cuts), largest / len(cuts))
        loudness = loudness * jnp.repeat(jnp.exp(heights), extent[axis_at] // parts).reshape((-1,) + (1,) * (len(extent) - 1 - axis_at))
    return loudness


def normal_values(key, extent, spread, most, cuts=(), kind=jnp.bfloat16):
    factor_of = block_levels(key, extent, cuts, -0.22, 0.18) if cuts else 1.0
    array = jax.random.normal(key, extent, jnp.float32) * spread * factor_of
    return jnp.minimum(jnp.maximum(array, -most), most).astype(kind)


def setup_inputs(seed: int = 0) -> dict:
    seeds = jax.random.split(jax.random.key(seed), 14)
    saved_input = draw_saved_input(jax.random.fold_in(seeds[13], 71), 0)
    query_cotangent = normal_values(seeds[1], (TOKENS, QW), (0.3 / TOKENS ** 0.5), 0.0049438477, ((0, 128), (1, 2)))
    key_cotangent = normal_values(seeds[2], (TOKENS, KW), (0.3 / TOKENS ** 0.5), 0.0049438477, ((0, 128), (1, 2)))
    query_weight = draw_query_weight(jax.random.fold_in(seeds[13], 71), 0)
    key_weight = draw_key_weight(jax.random.fold_in(seeds[13], 71), 0)
    query_moment = draw_query_moment(jax.random.fold_in(seeds[13], 71), 0)
    key_moment = draw_key_moment(jax.random.fold_in(seeds[13], 71), 0)
    query_row_root = draw_query_row_root(jax.random.fold_in(seeds[13], 71), 0)
    key_row_root = draw_key_row_root(jax.random.fold_in(seeds[13], 71), 0)
    query_head_root = draw_query_head_root(jax.random.fold_in(seeds[13], 71), 0)
    key_head_root = draw_key_head_root(jax.random.fold_in(seeds[13], 71), 0)
    query_head_stat = draw_query_head_stat(jax.random.fold_in(seeds[13], 71), 0)
    key_head_stat = draw_key_head_stat(jax.random.fold_in(seeds[13], 71), 0)
    return dict(saved_input=saved_input, query_cotangent=query_cotangent, key_cotangent=key_cotangent, query_weight=query_weight, key_weight=key_weight, query_moment=query_moment, key_moment=key_moment, query_row_root=query_row_root, key_row_root=key_row_root, query_head_root=query_head_root, key_head_root=key_head_root, query_head_stat=query_head_stat, key_head_stat=key_head_stat)


MOMENT_DECAY = 0.8
STAT_DECAY = 0.5
LEARN_RATE = 0.1
EPSILON = 1e-06

def update(gradient, weight, moment, stat, row_root, head_root):
    row_total = gradient.shape[0]
    head_count = head_root.shape[0]
    rounded = lax.optimization_barrier(gradient.astype(jnp.bfloat16)).astype(jnp.float32)
    shaped = rounded.reshape(row_total, head_count, HEAD_DIM)
    gram = jnp.einsum('rhd,rhe->hde', shaped, shaped)
    stat_next = STAT_DECAY * stat + (1.0 - STAT_DECAY) * gram / D
    rightward = jnp.einsum('rhd,hde->rhe', shaped, head_root.astype(jnp.float32))
    rightward = rightward.reshape(row_total, head_count * HEAD_DIM).astype(jnp.bfloat16)
    preconditioned = jnp.dot(row_root, rightward, preferred_element_type=jnp.float32)
    moment_next = MOMENT_DECAY * moment + (1.0 - MOMENT_DECAY) * preconditioned
    trust_ratio = jnp.sqrt(jnp.sum(weight * weight)) / jnp.sqrt(jnp.sum(moment_next * moment_next) + EPSILON)
    update_step = LEARN_RATE * trust_ratio * moment_next
    weight_next = weight - update_step
    return (update_step, weight_next, weight_next.astype(jnp.bfloat16), moment_next, stat_next)

def token_sum(saved_input, cotangent):
    return lax.dot_general(saved_input, cotangent, (((0,), (0,)), ((), ())), preferred_element_type=jnp.float32)

def reference(saved_input, query_cotangent, key_cotangent, query_weight, key_weight, query_moment, key_moment, query_row_root, key_row_root, query_head_root, key_head_root, query_head_stat, key_head_stat):
    query_out = update(token_sum(saved_input, query_cotangent), query_weight, query_moment, query_head_stat, query_row_root, query_head_root)
    key_out = update(token_sum(saved_input, key_cotangent), key_weight, key_moment, key_head_stat, key_row_root, key_head_root)
    return (query_out[0], key_out[0], query_out[1], key_out[1], query_out[2], key_out[2], query_out[3], key_out[3], query_out[4], key_out[4])
```

```python
import jax
import jax.numpy as jnp
from jax import lax
from jax.sharding import Mesh
from jax.sharding import PartitionSpec as P

D = 2048
HEAD_DIM = 64
MOMENT_DECAY = 0.8
STAT_DECAY = 0.5
LEARN_RATE = 0.1
EPSILON = 1e-06

XY = ("x", "yh", "yl")
QROWS = 128
KROWS = 32
BLOCK = QROWS + KROWS
PAIR = 2 * HEAD_DIM


def shifted(value, axis, shift):
    count = lax.axis_size(axis)
    return lax.ppermute(value, axis, [(i, (i + shift) % count) for i in range(count)])


def to_everyone(value, axes):
    count = lax.axis_size(axes)
    return lax.all_to_all(
        jnp.broadcast_to(value[None], (count, *value.shape)), axes, 0, 0, tiled=True
    )


def neighbours_x(value):
    return jnp.stack([value] + [shifted(value, "x", -s) for s in (1, 2, 3)])


def ring_z(value):
    up, down = value, value
    ahead, behind = [], []
    for _ in range(3):
        up = shifted(up, "z", -1)
        ahead.append(up)
    for _ in range(4):
        down = shifted(down, "z", 1)
        behind.append(down)
    return jnp.stack([value] + ahead + behind[::-1])


def from_first(parts, at, count):
    whole = jnp.concatenate([parts] * 2)
    start = (len(parts) - at) % len(parts)
    return lax.dynamic_slice_in_dim(whole, start, count, axis=0)


def in_pairs(value):
    return jnp.stack(jnp.split(value, value.shape[-1] // PAIR, axis=-1))


def side_by_side(parts):
    return jnp.concatenate(list(parts), axis=-1)


def in_heads(pairs):
    heads = jnp.stack([pairs[..., :HEAD_DIM], pairs[..., HEAD_DIM:]], 1)
    return heads.reshape(-1, HEAD_DIM, HEAD_DIM)


def one_of(value, index, axis):
    return lax.dynamic_index_in_dim(value, index, axis, keepdims=False)


def pair_root(roots, pair):
    two = lax.dynamic_slice_in_dim(roots, 2 * pair, 2, axis=0)
    none = jnp.zeros_like(two[0])
    return jnp.concatenate(
        [jnp.concatenate([two[0], none], 1), jnp.concatenate([none, two[1]], 1)], 0
    )


def pair_gram(rounded):
    both = lax.dot_general(
        rounded, rounded, (((0,), (0,)), ((), ())), preferred_element_type=jnp.float32
    )
    first = lax.broadcasted_iota(jnp.int32, both.shape, 0) < HEAD_DIM
    own = first == (lax.broadcasted_iota(jnp.int32, both.shape, 1) < HEAD_DIM)
    both = jnp.where(own, both, 0.0)
    return both[:HEAD_DIM] + both[HEAD_DIM:]


def column_factor(rounded, root):
    return jnp.dot(rounded, root, preferred_element_type=jnp.float32).astype(jnp.bfloat16)


def token_sum(saved_input, cotangent):
    return lax.dot_general(
        saved_input, cotangent, (((0,), (0,)), ((), ())), preferred_element_type=jnp.float32
    )


def shards(
    saved_input,
    query_cotangent,
    key_cotangent,
    query_weight,
    key_weight,
    query_moment,
    key_moment,
    query_row_root,
    key_row_root,
    query_head_root,
    key_head_root,
    query_head_stat,
    key_head_stat,
):
    f32 = jnp.float32
    z, x = lax.axis_index("z"), lax.axis_index("x")
    yh, yl = lax.axis_index("yh"), lax.axis_index("yl")

    query_part = in_pairs(token_sum(saved_input, query_cotangent))
    query_part = query_part.reshape(4, 2, 8, 2, QROWS, PAIR).transpose(0, 1, 3, 2, 4, 5)
    key_part = in_pairs(token_sum(saved_input, key_cotangent))
    key_part = key_part.reshape(2, 8, 4, 2, KROWS, PAIR).transpose(2, 0, 3, 1, 4, 5)
    part = jnp.concatenate(
        [query_part.reshape(16, 8, QROWS, PAIR), key_part.reshape(16, 8, KROWS, PAIR)], axis=2
    )
    part = part.reshape(16, 8 * BLOCK, PAIR)

    query_rows = from_first(neighbours_x(query_row_root), x - 2 * yl, 2)
    key_rows = lax.dynamic_slice_in_dim(key_row_root, yl * KROWS, KROWS, axis=0)
    roots = jnp.concatenate([query_rows.reshape(QROWS, D), key_rows], 0)
    both = jnp.stack([in_pairs(query_moment), in_pairs(query_weight)], 1)
    both = one_of(both.reshape(4, 2, 2, HEAD_DIM, PAIR), yh, 1)
    both = lax.all_to_all(both, "x", 0, 0, tiled=True)
    both = lax.dynamic_slice_in_dim(both, 2 * yl, 2, axis=0)
    query_both = both.transpose(1, 0, 2, 3).reshape(2, QROWS, PAIR)
    key_both = one_of(jnp.stack([in_pairs(key_moment), in_pairs(key_weight)], 1), yh, 0)
    key_both = lax.dynamic_slice_in_dim(key_both, yl * KROWS, KROWS, axis=1)
    state = jnp.concatenate([query_both, key_both], 1)
    all_roots = ring_z(roots)
    all_state = ring_z(state)
    query_roots = all_roots[:, :QROWS].reshape(8 * QROWS, D)
    key_roots = all_roots[:, QROWS:].reshape(8 * KROWS, D)
    moment, weight = all_state[:, 0], all_state[:, 1]

    summed = lax.psum_scatter(part, XY, scatter_dimension=0, tiled=True)
    arrived = lax.all_to_all(summed.reshape(8, BLOCK, PAIR), "z", 0, 0, tiled=True)
    rounded = arrived.sum(axis=0).astype(jnp.bfloat16)
    rounded = to_everyone(rounded, ("z", "yl"))
    query_rounded = rounded[:, :QROWS].reshape(D, PAIR)
    key_rounded = rounded[:, QROWS:].reshape(512, PAIR)
    key_rounded = from_first(neighbours_x(key_rounded), x, 4)
    key_rounded = key_rounded.reshape(4, 8, 64, PAIR).transpose(1, 0, 2, 3).reshape(D, PAIR)

    query_gram = pair_gram(query_rounded)
    key_gram = pair_gram(key_rounded)
    query_right = column_factor(query_rounded, pair_root(query_head_root, 2 * x + yh))
    key_right = column_factor(key_rounded, pair_root(key_head_root, yh))
    query_pre = jnp.dot(query_roots, query_right, preferred_element_type=f32)
    key_pre = jnp.dot(key_roots, key_right, preferred_element_type=f32)
    pre = jnp.concatenate(
        [query_pre.reshape(8, QROWS, PAIR), key_pre.reshape(8, KROWS, PAIR)], 1
    )
    moment_next = MOMENT_DECAY * moment + (1.0 - MOMENT_DECAY) * pre

    squares = jnp.stack([moment_next * moment_next, weight * weight])
    sums = jnp.stack(
        [jnp.sum(squares[:, :, :QROWS], (1, 2, 3)), jnp.sum(squares[:, :, QROWS:], (1, 2, 3))]
    )
    sums = to_everyone(sums.reshape(1, 4), (*XY, "c")).sum(axis=(0, 1)).reshape(2, 2)
    rate = LEARN_RATE * (jnp.sqrt(sums[:, 1]) / jnp.sqrt(sums[:, 0] + EPSILON))

    rates = jnp.concatenate([jnp.full((QROWS, 1), rate[0]), jnp.full((KROWS, 1), rate[1])])
    copies = (weight - rates * moment_next).astype(jnp.bfloat16)
    copies = from_first(copies, z, 8).reshape(8 * BLOCK, PAIR)
    copies = lax.all_gather(copies, XY, axis=0, tiled=True)
    copies = copies.reshape(4, 2, 2, 8, BLOCK, PAIR)
    query_copy = copies[:, :, :, :, :QROWS].transpose(0, 1, 3, 2, 4, 5)
    query_copy = side_by_side(query_copy.reshape(8, D, PAIR))
    key_copy = copies[:, :, :, :, QROWS:].transpose(1, 3, 0, 2, 4, 5)
    key_copy = side_by_side(key_copy.reshape(2, D, PAIR))

    query_mine = moment_next[0, :QROWS].reshape(1, 2, 1, HEAD_DIM, PAIR)
    query_mine = jnp.broadcast_to(query_mine, (2, 2, 4, HEAD_DIM, PAIR))
    others = jnp.concatenate(
        [
            moment_next[0, QROWS:],
            lax.dynamic_slice_in_dim(query_gram, 32 * yl, 32, axis=0),
            lax.dynamic_slice_in_dim(key_gram, 8 * (2 * x + yl), 8, axis=0),
        ]
    )
    others = jnp.broadcast_to(others, (16, *others.shape))
    sent = jnp.concatenate([query_mine.reshape(16, HEAD_DIM, PAIR), others], 1)
    got = lax.all_to_all(sent, XY, 0, 0, tiled=True).reshape(4, 2, 2, 136, PAIR)
    query_moment_next = one_of(got[:, :, :, :64], x // 2, 2)
    query_moment_next = side_by_side(query_moment_next.reshape(8, HEAD_DIM, PAIR))
    key_moment_next = one_of(got[:, :, :, 64:96], x, 0)
    key_moment_next = side_by_side(key_moment_next.reshape(2, HEAD_DIM, PAIR))
    query_total = in_heads(got[:, :, :, 96:128].reshape(8, HEAD_DIM, PAIR))
    key_total = got[:, :, :, 128:].transpose(1, 0, 2, 3, 4)
    key_total = in_heads(key_total.reshape(2, HEAD_DIM, PAIR))

    query_step = rate[0] * query_moment_next
    key_step = rate[1] * key_moment_next
    return (
        query_step,
        key_step,
        query_weight - query_step,
        key_weight - key_step,
        query_copy,
        key_copy,
        query_moment_next,
        key_moment_next,
        STAT_DECAY * query_head_stat + (1.0 - STAT_DECAY) * query_total / D,
        STAT_DECAY * key_head_stat + (1.0 - STAT_DECAY) * key_total / D,
    )


def solution(mesh):
    split = Mesh(mesh.devices.reshape(8, 4, 2, 2, 2), ("z", "x", "yh", "yl", "c"))
    tokens = ("z", "x", "yh", "yl")
    rows = P(("z", "x"), "c")
    heads = P("c", None, None)
    placed = (P(tokens, None), P(tokens, "c"), P(tokens, "c"), rows, rows, rows, rows)
    placed += (P(("z", "x"), None),) * 2 + (heads,) * 4
    whole = P(None, "c")
    return jax.shard_map(
        shards,
        mesh=split,
        in_specs=placed,
        out_specs=(rows, rows, rows, rows, whole, whole, rows, rows, heads, heads),
        check_vma=False,
    )
```

```python
import jax
import jax.numpy as jnp
from jax import lax
from jax.experimental import pallas as pl
from jax.experimental.pallas import tpu as pltpu
from jax.sharding import Mesh
from jax.sharding import PartitionSpec as P

D = 2048
HEAD_DIM = 64
MOMENT_DECAY = 0.8
STAT_DECAY = 0.5
LEARN_RATE = 0.1
EPSILON = 1e-06

XY = ("x", "yh", "yl")
QROWS = 128
KROWS = 32
BLOCK = QROWS + KROWS
PAIR = 2 * HEAD_DIM


def shifted(value, axis, shift):
    count = lax.axis_size(axis)
    return lax.ppermute(value, axis, [(i, (i + shift) % count) for i in range(count)])


def to_everyone(value, axes):
    count = lax.axis_size(axes)
    return lax.all_to_all(
        jnp.broadcast_to(value[None], (count, *value.shape)), axes, 0, 0, tiled=True
    )


def neighbours_x(value):
    return [value] + [shifted(value, "x", -s) for s in (1, 2, 3)]


def ring_z(value):
    up, down = value, value
    ahead, behind = [], []
    for _ in range(3):
        up = shifted(up, "z", -1)
        ahead.append(up)
    for _ in range(4):
        down = shifted(down, "z", 1)
        behind.append(down)
    return jnp.stack([value] + ahead + behind[::-1])


def picked(parts, index):
    index = index % len(parts)
    value = parts[0]
    for i in range(1, len(parts)):
        value = jnp.where(index == i, parts[i], value)
    return value


def in_pairs(value):
    return jnp.stack(jnp.split(value, value.shape[-1] // PAIR, axis=-1))


def side_by_side(parts):
    return jnp.concatenate(list(parts), axis=-1)


def in_heads(pairs):
    heads = jnp.stack([pairs[..., :HEAD_DIM], pairs[..., HEAD_DIM:]], 1)
    return heads.reshape(-1, HEAD_DIM, HEAD_DIM)


def one_of(value, index, axis):
    return lax.dynamic_index_in_dim(value, index, axis, keepdims=False)


def pair_root(roots, pair):
    two = lax.dynamic_slice_in_dim(roots, 2 * pair, 2, axis=0)
    none = jnp.zeros_like(two[0])
    return jnp.concatenate(
        [jnp.concatenate([two[0], none], 1), jnp.concatenate([none, two[1]], 1)], 0
    )


def pair_gram(rounded):
    both = lax.dot_general(
        rounded, rounded, (((0,), (0,)), ((), ())), preferred_element_type=jnp.float32
    )
    first = lax.broadcasted_iota(jnp.int32, both.shape, 0) < HEAD_DIM
    own = first == (lax.broadcasted_iota(jnp.int32, both.shape, 1) < HEAD_DIM)
    both = jnp.where(own, both, 0.0)
    return both[:HEAD_DIM] + both[HEAD_DIM:]


def square_sums(value):
    squares = value * value
    return jnp.sum(squares[:, :QROWS]), jnp.sum(squares[:, QROWS:])


def column_factor(rounded, root):
    return jnp.dot(rounded, root, preferred_element_type=jnp.float32).astype(jnp.bfloat16)


def token_sum_body(input_ref, query_ref, key_ref, part_ref, turned_ref, key_sum_ref):
    x = pl.program_id(0)

    @pl.when(x == 0)
    def _():
        for row in range(0, D, 256):
            turned_ref[row : row + 256, :] = input_ref[:, row : row + 256].T
        key_sum_ref[...] = jnp.dot(
            turned_ref[...], key_ref[...], preferred_element_type=jnp.float32
        )

    query_sum = jnp.dot(turned_ref[...], query_ref[...], preferred_element_type=jnp.float32)
    for yh in range(2):
        lanes = slice(yh * PAIR, (yh + 1) * PAIR)
        for yl in range(2):
            for z in range(8):
                row = z * 256 + yl * QROWS
                part_ref[2 * yh + yl, z, :QROWS, :] = query_sum[row : row + QROWS, lanes]
                row = pl.multiple_of(z * 256 + x * 64 + yl * KROWS, KROWS)
                part_ref[2 * yh + yl, z, QROWS:, :] = key_sum_ref[pl.ds(row, KROWS), lanes]


def token_sums(saved_input, query_cotangent, key_cotangent):
    tokens = saved_input.shape[0]
    return pl.pallas_call(
        token_sum_body,
        grid=(4,),
        in_specs=[
            pl.BlockSpec((tokens, D), lambda x: (0, 0)),
            pl.BlockSpec((tokens, 2 * PAIR), lambda x: (0, x)),
            pl.BlockSpec((tokens, 2 * PAIR), lambda x: (0, 0)),
        ],
        out_specs=pl.BlockSpec((4, 8, BLOCK, PAIR), lambda x: (x, 0, 0, 0)),
        out_shape=jax.ShapeDtypeStruct((16, 8, BLOCK, PAIR), jnp.float32),
        scratch_shapes=[
            pltpu.VMEM((D, tokens), jnp.bfloat16),
            pltpu.VMEM((D, 2 * PAIR), jnp.float32),
        ],
        compiler_params=pltpu.CompilerParams(vmem_limit_bytes=48 * 1024 * 1024),
        cost_estimate=pl.CostEstimate(
            flops=2 * tokens * D * 10 * PAIR, bytes_accessed=17 * 2**20, transcendentals=0
        ),
    )(saved_input, query_cotangent, key_cotangent)


def placed_body(z_ref, blocks_ref, query_ref, key_ref):
    for x in range(4):
        for yh in range(2):
            for yl in range(2):
                block = 4 * x + 2 * yh + yl
                lanes = slice((2 * x + yh) * PAIR, (2 * x + yh + 1) * PAIR)
                query_ref[yl * QROWS : (yl + 1) * QROWS, lanes] = blocks_ref[block, 0, :QROWS, :]
                row = x * 64 + yl * KROWS
                lanes = slice(yh * PAIR, (yh + 1) * PAIR)
                key_ref[row : row + KROWS, lanes] = blocks_ref[block, 0, QROWS:, :]


def placed_copies(blocks, z):
    return pl.pallas_call(
        placed_body,
        grid_spec=pltpu.PrefetchScalarGridSpec(
            num_scalar_prefetch=1,
            grid=(8,),
            in_specs=[
                pl.BlockSpec(
                    (16, 1, BLOCK, PAIR), lambda i, z_ref: (0, lax.rem(i + 8 - z_ref[0], 8), 0, 0)
                )
            ],
            out_specs=[
                pl.BlockSpec((256, 8 * PAIR), lambda i, z_ref: (i, 0)),
                pl.BlockSpec((256, 2 * PAIR), lambda i, z_ref: (i, 0)),
            ],
        ),
        out_shape=[
            jax.ShapeDtypeStruct((D, 8 * PAIR), jnp.bfloat16),
            jax.ShapeDtypeStruct((D, 2 * PAIR), jnp.bfloat16),
        ],
    )(z.reshape(1).astype(jnp.int32), blocks)


def shards(
    saved_input,
    query_cotangent,
    key_cotangent,
    query_weight,
    key_weight,
    query_moment,
    key_moment,
    query_row_root,
    key_row_root,
    query_head_root,
    key_head_root,
    query_head_stat,
    key_head_stat,
):
    f32 = jnp.float32
    z, x = lax.axis_index("z"), lax.axis_index("x")
    yh, yl = lax.axis_index("yh"), lax.axis_index("yl")

    part = token_sums(saved_input, query_cotangent, key_cotangent)
    part = part.reshape(16, 8 * BLOCK, PAIR)

    query_rows = neighbours_x(query_row_root)
    query_rows = [picked(query_rows, 2 * yl + j - x + 4) for j in range(2)]
    key_rows = lax.dynamic_slice_in_dim(key_row_root, yl * KROWS, KROWS, axis=0)
    roots = jnp.concatenate([*query_rows, key_rows], 0)
    both = jnp.stack([in_pairs(query_moment), in_pairs(query_weight)], 1)
    both = one_of(both.reshape(4, 2, 2, HEAD_DIM, PAIR), yh, 1)
    both = lax.all_to_all(both, "x", 0, 0, tiled=True)
    both = lax.dynamic_slice_in_dim(both, 2 * yl, 2, axis=0)
    query_both = both.transpose(1, 0, 2, 3).reshape(2, QROWS, PAIR)
    key_both = one_of(jnp.stack([in_pairs(key_moment), in_pairs(key_weight)], 1), yh, 0)
    key_both = lax.dynamic_slice_in_dim(key_both, yl * KROWS, KROWS, axis=1)
    state = jnp.concatenate([query_both, key_both], 1)
    all_roots = ring_z(roots)
    all_state = ring_z(state)
    query_roots = all_roots[:, :QROWS].reshape(8 * QROWS, D)
    key_roots = all_roots[:, QROWS:].reshape(8 * KROWS, D)
    moment, weight = all_state[:, 0], all_state[:, 1]

    summed = lax.psum_scatter(part, XY, scatter_dimension=0, tiled=True)
    arrived = lax.all_to_all(summed.reshape(8, BLOCK, PAIR), "z", 0, 0, tiled=True)
    rounded = arrived.sum(axis=0).astype(jnp.bfloat16)
    rounded = to_everyone(rounded, ("z", "yl"))
    query_rounded = rounded[:, :QROWS].reshape(D, PAIR)
    key_rounded = rounded[:, QROWS:].reshape(512, PAIR)
    key_rounded = neighbours_x(key_rounded.reshape(8, 64, PAIR))
    key_rounded = jnp.stack([picked(key_rounded, j - x + 4) for j in range(4)], 1)
    key_rounded = key_rounded.reshape(D, PAIR)

    query_gram = pair_gram(query_rounded)
    key_gram = pair_gram(key_rounded)
    query_right = column_factor(query_rounded, pair_root(query_head_root, 2 * x + yh))
    key_right = column_factor(key_rounded, pair_root(key_head_root, yh))
    query_pre = jnp.dot(query_roots, query_right, preferred_element_type=f32)
    key_pre = jnp.dot(key_roots, key_right, preferred_element_type=f32)
    pre = jnp.concatenate(
        [query_pre.reshape(8, QROWS, PAIR), key_pre.reshape(8, KROWS, PAIR)], 1
    )
    moment_next = MOMENT_DECAY * moment + (1.0 - MOMENT_DECAY) * pre

    sums = jnp.stack([*square_sums(moment_next), *square_sums(weight)]).reshape(1, 4)
    sums = sums + shifted(sums, "c", 1)
    sums = to_everyone(sums, XY).sum(axis=(0, 1)).reshape(2, 2)
    rate = LEARN_RATE * (jnp.sqrt(sums[1]) / jnp.sqrt(sums[0] + EPSILON))

    rates = jnp.concatenate([jnp.full((QROWS, 1), rate[0]), jnp.full((KROWS, 1), rate[1])])
    copies = (weight - rates * moment_next).astype(jnp.bfloat16)
    copies = lax.all_gather(copies.reshape(8 * BLOCK, PAIR), XY, axis=0, tiled=True)
    query_copy, key_copy = placed_copies(copies.reshape(16, 8, BLOCK, PAIR), z)

    query_mine = moment_next[0, :QROWS].reshape(1, 2, 1, HEAD_DIM, PAIR)
    query_mine = jnp.broadcast_to(query_mine, (2, 2, 4, HEAD_DIM, PAIR))
    others = jnp.concatenate(
        [
            moment_next[0, QROWS:],
            lax.dynamic_slice_in_dim(query_gram, 32 * yl, 32, axis=0),
            lax.dynamic_slice_in_dim(key_gram, 8 * (2 * x + yl), 8, axis=0),
        ]
    )
    others = jnp.broadcast_to(others, (16, *others.shape))
    sent = jnp.concatenate([query_mine.reshape(16, HEAD_DIM, PAIR), others], 1)
    got = lax.all_to_all(sent, XY, 0, 0, tiled=True).reshape(4, 2, 2, 136, PAIR)
    query_moment_next = one_of(got[:, :, :, :64], x // 2, 2)
    query_moment_next = side_by_side(query_moment_next.reshape(8, HEAD_DIM, PAIR))
    key_moment_next = one_of(got[:, :, :, 64:96], x, 0)
    key_moment_next = side_by_side(key_moment_next.reshape(2, HEAD_DIM, PAIR))
    query_total = in_heads(got[:, :, :, 96:128].reshape(8, HEAD_DIM, PAIR))
    key_total = got[:, :, :, 128:].transpose(1, 0, 2, 3, 4)
    key_total = in_heads(key_total.reshape(2, HEAD_DIM, PAIR))

    query_step = rate[0] * query_moment_next
    key_step = rate[1] * key_moment_next
    return (
        query_step,
        key_step,
        query_weight - query_step,
        key_weight - key_step,
        query_copy,
        key_copy,
        query_moment_next,
        key_moment_next,
        STAT_DECAY * query_head_stat + (1.0 - STAT_DECAY) * query_total / D,
        STAT_DECAY * key_head_stat + (1.0 - STAT_DECAY) * key_total / D,
    )


def solution(mesh):
    split = Mesh(mesh.devices.reshape(8, 4, 2, 2, 2), ("z", "x", "yh", "yl", "c"))
    tokens = ("z", "x", "yh", "yl")
    rows = P(("z", "x"), "c")
    heads = P("c", None, None)
    placed = (P(tokens, None), P(tokens, "c"), P(tokens, "c"), rows, rows, rows, rows)
    placed += (P(("z", "x"), None),) * 2 + (heads,) * 4
    whole = P(None, "c")
    return jax.shard_map(
        shards,
        mesh=split,
        in_specs=placed,
        out_specs=(rows, rows, rows, rows, whole, whole, rows, rows, heads, heads),
        check_vma=False,
    )
```

```python
import functools

import jax
import jax.numpy as jnp
from jax import lax
from jax.experimental import pallas as pl
from jax.experimental.pallas import tpu as pltpu
from jax.sharding import Mesh
from jax.sharding import PartitionSpec as P

D = 2048
HEAD_DIM = 64
MOMENT_DECAY = 0.8
STAT_DECAY = 0.5
LEARN_RATE = 0.1
EPSILON = 1e-06

XY = ("x", "yh", "yl")
QROWS = 128
KROWS = 32
BLOCK = QROWS + KROWS
PAIR = 2 * HEAD_DIM


def shifted(value, axis, shift):
    count = lax.axis_size(axis)
    return lax.ppermute(value, axis, [(i, (i + shift) % count) for i in range(count)])


def to_everyone(value, axes):
    count = lax.axis_size(axes)
    return lax.all_to_all(
        jnp.broadcast_to(value[None], (count, *value.shape)), axes, 0, 0, tiled=True
    )


def neighbours_x(value):
    return [value] + [shifted(value, "x", -s) for s in (1, 2, 3)]


def ring_z(value):
    up, down = value, value
    ahead, behind = [], []
    for _ in range(3):
        up = shifted(up, "z", -1)
        ahead.append(up)
    for _ in range(4):
        down = shifted(down, "z", 1)
        behind.append(down)
    return jnp.stack([value] + ahead + behind[::-1])


def picked(parts, index):
    index = index % len(parts)
    value = parts[0]
    for i in range(1, len(parts)):
        value = jnp.where(index == i, parts[i], value)
    return value


def in_pairs(value):
    return jnp.stack(jnp.split(value, value.shape[-1] // PAIR, axis=-1))


def side_by_side(parts):
    return jnp.concatenate(list(parts), axis=-1)


def in_heads(pairs):
    heads = jnp.stack([pairs[..., :HEAD_DIM], pairs[..., HEAD_DIM:]], 1)
    return heads.reshape(-1, HEAD_DIM, HEAD_DIM)


def one_of(value, index, axis):
    return lax.dynamic_index_in_dim(value, index, axis, keepdims=False)


def pair_root(roots, pair):
    two = lax.dynamic_slice_in_dim(roots, 2 * pair, 2, axis=0)
    none = jnp.zeros_like(two[0])
    return jnp.concatenate(
        [jnp.concatenate([two[0], none], 1), jnp.concatenate([none, two[1]], 1)], 0
    )


def pair_gram(rounded):
    both = lax.dot_general(
        rounded, rounded, (((0,), (0,)), ((), ())), preferred_element_type=jnp.float32
    )
    first = lax.broadcasted_iota(jnp.int32, both.shape, 0) < HEAD_DIM
    own = first == (lax.broadcasted_iota(jnp.int32, both.shape, 1) < HEAD_DIM)
    both = jnp.where(own, both, 0.0)
    return both[:HEAD_DIM] + both[HEAD_DIM:]


def token_sum_body(input_ref, query_ref, key_ref, part_ref, turned_ref, key_sum_ref):
    x = pl.program_id(0)

    @pl.when(x == 0)
    def _():
        for row in range(0, D, 256):
            turned_ref[row : row + 256, :] = input_ref[:, row : row + 256].T
        key_sum_ref[...] = jnp.dot(
            turned_ref[...], key_ref[...], preferred_element_type=jnp.float32
        )

    query_sum = jnp.dot(turned_ref[...], query_ref[...], preferred_element_type=jnp.float32)
    for yh in range(2):
        lanes = slice(yh * PAIR, (yh + 1) * PAIR)
        for yl in range(2):
            for z in range(8):
                row = z * 256 + yl * QROWS
                part_ref[2 * yh + yl, z, :QROWS, :] = query_sum[row : row + QROWS, lanes]
                row = pl.multiple_of(z * 256 + x * 64 + yl * KROWS, KROWS)
                part_ref[2 * yh + yl, z, QROWS:, :] = key_sum_ref[pl.ds(row, KROWS), lanes]


def token_sums(saved_input, query_cotangent, key_cotangent):
    tokens = saved_input.shape[0]
    return pl.pallas_call(
        token_sum_body,
        grid=(4,),
        in_specs=[
            pl.BlockSpec((tokens, D), lambda x: (0, 0)),
            pl.BlockSpec((tokens, 2 * PAIR), lambda x: (0, x)),
            pl.BlockSpec((tokens, 2 * PAIR), lambda x: (0, 0)),
        ],
        out_specs=pl.BlockSpec((4, 8, BLOCK, PAIR), lambda x: (x, 0, 0, 0)),
        out_shape=jax.ShapeDtypeStruct((16, 8, BLOCK, PAIR), jnp.float32),
        scratch_shapes=[
            pltpu.VMEM((D, tokens), jnp.bfloat16),
            pltpu.VMEM((D, 2 * PAIR), jnp.float32),
        ],
        compiler_params=pltpu.CompilerParams(vmem_limit_bytes=48 * 1024 * 1024),
        cost_estimate=pl.CostEstimate(
            flops=2 * tokens * D * 10 * PAIR, bytes_accessed=17 * 2**20, transcendentals=0
        ),
    )(saved_input, query_cotangent, key_cotangent)


def moment_body(
    first,
    roots_ref,
    rounded_ref,
    root_ref,
    state_ref,
    next_ref,
    sums_ref,
    right_ref,
    squares_ref,
):
    step = pl.program_id(0)

    @pl.when(step == 0)
    def _():
        for i in range(D // QROWS):
            right = jnp.dot(rounded_ref[i], root_ref[...], preferred_element_type=jnp.float32)
            right_ref[i * QROWS : (i + 1) * QROWS, :] = right.astype(jnp.bfloat16)
        squares_ref[...] = jnp.zeros_like(squares_ref)

    roots = roots_ref[...].reshape(-1, D)
    pre = jnp.dot(roots, right_ref[...], preferred_element_type=jnp.float32)
    moment, weight = state_ref[:, 0], state_ref[:, 1]
    moment = MOMENT_DECAY * moment + (1.0 - MOMENT_DECAY) * pre.reshape(moment.shape)
    next_ref[...] = moment
    for i, value in enumerate((moment, weight)):
        squares_ref[i] += (value * value).reshape(-1, 8, PAIR).sum(axis=0)

    @pl.when(step == pl.num_programs(0) - 1)
    def _():
        row = lax.broadcasted_iota(jnp.int32, (8, PAIR), 0)
        of_weight = jnp.where(row == first + 1, jnp.sum(squares_ref[1]), 0.0)
        sums_ref[...] = jnp.where(row == first, jnp.sum(squares_ref[0]), of_weight)


def moment_update(roots, rounded, head_root, state, at, rows, first, blocks):
    return pl.pallas_call(
        functools.partial(moment_body, first),
        grid=(8 // blocks,),
        in_specs=[
            pl.BlockSpec((blocks, rows, D), lambda i: (i, at // rows, 0)),
            pl.BlockSpec((D // QROWS, QROWS, PAIR), lambda i: (0, 0, 0)),
            pl.BlockSpec((PAIR, PAIR), lambda i: (0, 0)),
            pl.BlockSpec((blocks, 2, rows, PAIR), lambda i: (i, 0, at // rows, 0)),
        ],
        out_specs=[
            pl.BlockSpec((blocks, rows, PAIR), lambda i: (i, 0, 0)),
            pl.BlockSpec((8, PAIR), lambda i: (0, 0)),
        ],
        out_shape=[
            jax.ShapeDtypeStruct((8, rows, PAIR), jnp.float32),
            jax.ShapeDtypeStruct((8, PAIR), jnp.float32),
        ],
        scratch_shapes=[
            pltpu.VMEM((D, PAIR), jnp.bfloat16),
            pltpu.VMEM((2, 8, PAIR), jnp.float32),
        ],
        cost_estimate=pl.CostEstimate(
            flops=2 * 8 * rows * D * PAIR, bytes_accessed=48 * rows * D, transcendentals=0
        ),
    )(roots, rounded, head_root, state)


def copies_body(sums_ref, query_ref, key_ref, weight_ref, copies_ref, rates_ref):
    sums = sums_ref[...].sum(axis=0)
    rates = []
    for i in range(2):
        of_moment, of_weight = sums[2 * i : 2 * i + 1], sums[2 * i + 1 : 2 * i + 2]
        rates.append(LEARN_RATE * (jnp.sqrt(of_weight) / jnp.sqrt(of_moment + EPSILON)))
    query = weight_ref[:, 0, :QROWS, :] - rates[0] * query_ref[...]
    key = weight_ref[:, 0, QROWS:, :] - rates[1] * key_ref[...]
    copies_ref[:, :QROWS, :] = query.astype(jnp.bfloat16)
    copies_ref[:, QROWS:, :] = key.astype(jnp.bfloat16)
    row = lax.broadcasted_iota(jnp.int32, (8, PAIR), 0)
    rates_ref[...] = jnp.where(row == 0, rates[0], rates[1])


def new_copies(sums, query_moment, key_moment, state):
    return pl.pallas_call(
        copies_body,
        grid=(1,),
        in_specs=[
            pl.BlockSpec((16, 8, PAIR), lambda i: (0, 0, 0)),
            pl.BlockSpec((8, QROWS, PAIR), lambda i: (0, 0, 0)),
            pl.BlockSpec((8, KROWS, PAIR), lambda i: (0, 0, 0)),
            pl.BlockSpec((8, 1, BLOCK, PAIR), lambda i: (0, 1, 0, 0)),
        ],
        out_specs=[
            pl.BlockSpec((8, BLOCK, PAIR), lambda i: (0, 0, 0)),
            pl.BlockSpec((8, PAIR), lambda i: (0, 0)),
        ],
        out_shape=[
            jax.ShapeDtypeStruct((8, BLOCK, PAIR), jnp.bfloat16),
            jax.ShapeDtypeStruct((8, PAIR), jnp.float32),
        ],
    )(sums, query_moment, key_moment, state)


def placed_body(z_ref, blocks_ref, query_ref, key_ref):
    for x in range(4):
        for yh in range(2):
            for yl in range(2):
                block = 4 * x + 2 * yh + yl
                lanes = slice((2 * x + yh) * PAIR, (2 * x + yh + 1) * PAIR)
                query_ref[yl * QROWS : (yl + 1) * QROWS, lanes] = blocks_ref[block, 0, :QROWS, :]
                row = x * 64 + yl * KROWS
                lanes = slice(yh * PAIR, (yh + 1) * PAIR)
                key_ref[row : row + KROWS, lanes] = blocks_ref[block, 0, QROWS:, :]


def placed_copies(blocks, z):
    return pl.pallas_call(
        placed_body,
        grid_spec=pltpu.PrefetchScalarGridSpec(
            num_scalar_prefetch=1,
            grid=(8,),
            in_specs=[
                pl.BlockSpec(
                    (16, 1, BLOCK, PAIR), lambda i, z_ref: (0, lax.rem(i + 8 - z_ref[0], 8), 0, 0)
                )
            ],
            out_specs=[
                pl.BlockSpec((256, 8 * PAIR), lambda i, z_ref: (i, 0)),
                pl.BlockSpec((256, 2 * PAIR), lambda i, z_ref: (i, 0)),
            ],
        ),
        out_shape=[
            jax.ShapeDtypeStruct((D, 8 * PAIR), jnp.bfloat16),
            jax.ShapeDtypeStruct((D, 2 * PAIR), jnp.bfloat16),
        ],
    )(z.reshape(1).astype(jnp.int32), blocks)


def shards(
    saved_input,
    query_cotangent,
    key_cotangent,
    query_weight,
    key_weight,
    query_moment,
    key_moment,
    query_row_root,
    key_row_root,
    query_head_root,
    key_head_root,
    query_head_stat,
    key_head_stat,
):
    z, x = lax.axis_index("z"), lax.axis_index("x")
    yh, yl = lax.axis_index("yh"), lax.axis_index("yl")

    part = token_sums(saved_input, query_cotangent, key_cotangent)
    part = part.reshape(16, 8 * BLOCK, PAIR)

    query_rows = neighbours_x(query_row_root)
    query_rows = [picked(query_rows, 2 * yl + j - x + 4) for j in range(2)]
    key_rows = lax.dynamic_slice_in_dim(key_row_root, yl * KROWS, KROWS, axis=0)
    roots = jnp.concatenate([*query_rows, key_rows], 0)
    both = jnp.stack([in_pairs(query_moment), in_pairs(query_weight)], 1)
    both = one_of(both.reshape(4, 2, 2, HEAD_DIM, PAIR), yh, 1)
    both = lax.all_to_all(both, "x", 0, 0, tiled=True)
    both = lax.dynamic_slice_in_dim(both, 2 * yl, 2, axis=0)
    query_both = both.transpose(1, 0, 2, 3).reshape(2, QROWS, PAIR)
    key_both = one_of(jnp.stack([in_pairs(key_moment), in_pairs(key_weight)], 1), yh, 0)
    key_both = lax.dynamic_slice_in_dim(key_both, yl * KROWS, KROWS, axis=1)
    state = jnp.concatenate([query_both, key_both], 1)
    all_roots = ring_z(roots)
    all_state = ring_z(state)

    summed = lax.psum_scatter(part, XY, scatter_dimension=0, tiled=True)
    arrived = lax.all_to_all(summed.reshape(8, BLOCK, PAIR), "z", 0, 0, tiled=True)
    rounded = arrived.sum(axis=0).astype(jnp.bfloat16)
    rounded = to_everyone(rounded, ("z", "yl"))
    query_rounded = rounded[:, :QROWS].reshape(D, PAIR)
    key_rounded = rounded[:, QROWS:].reshape(512, PAIR)
    key_rounded = neighbours_x(key_rounded.reshape(8, 64, PAIR))
    key_rounded = jnp.stack([picked(key_rounded, j - x + 4) for j in range(4)], 1)
    key_rounded = key_rounded.reshape(D, PAIR)

    query_gram = pair_gram(query_rounded)
    key_gram = pair_gram(key_rounded)
    query_next, query_sums = moment_update(
        all_roots, rounded, pair_root(query_head_root, 2 * x + yh), all_state, 0, QROWS, 0, 4
    )
    key_next, key_sums = moment_update(
        all_roots,
        key_rounded.reshape(D // QROWS, QROWS, PAIR),
        pair_root(key_head_root, yh),
        all_state,
        QROWS,
        KROWS,
        2,
        8,
    )
    sums = query_sums + key_sums
    sums = to_everyone(sums + shifted(sums, "c", 1), XY)
    copies, rates = new_copies(sums, query_next, key_next, all_state)
    copies = lax.all_gather(copies.reshape(8 * BLOCK, PAIR), XY, axis=0, tiled=True)
    query_copy, key_copy = placed_copies(copies.reshape(16, 8, BLOCK, PAIR), z)

    query_mine = query_next[0].reshape(1, 2, 1, HEAD_DIM, PAIR)
    query_mine = jnp.broadcast_to(query_mine, (2, 2, 4, HEAD_DIM, PAIR))
    others = jnp.concatenate(
        [
            key_next[0],
            lax.dynamic_slice_in_dim(query_gram, 32 * yl, 32, axis=0),
            lax.dynamic_slice_in_dim(key_gram, 8 * (2 * x + yl), 8, axis=0),
        ]
    )
    others = jnp.broadcast_to(others, (16, *others.shape))
    sent = jnp.concatenate([query_mine.reshape(16, HEAD_DIM, PAIR), others], 1)
    got = lax.all_to_all(sent, XY, 0, 0, tiled=True).reshape(4, 2, 2, 136, PAIR)
    query_moment_next = one_of(got[:, :, :, :64], x // 2, 2)
    query_moment_next = side_by_side(query_moment_next.reshape(8, HEAD_DIM, PAIR))
    key_moment_next = one_of(got[:, :, :, 64:96], x, 0)
    key_moment_next = side_by_side(key_moment_next.reshape(2, HEAD_DIM, PAIR))
    query_total = in_heads(got[:, :, :, 96:128].reshape(8, HEAD_DIM, PAIR))
    key_total = got[:, :, :, 128:].transpose(1, 0, 2, 3, 4)
    key_total = in_heads(key_total.reshape(2, HEAD_DIM, PAIR))

    query_step = rates[0, 0] * query_moment_next
    key_step = rates[1, 0] * key_moment_next
    return (
        query_step,
        key_step,
        query_weight - query_step,
        key_weight - key_step,
        query_copy,
        key_copy,
        query_moment_next,
        key_moment_next,
        STAT_DECAY * query_head_stat + (1.0 - STAT_DECAY) * query_total / D,
        STAT_DECAY * key_head_stat + (1.0 - STAT_DECAY) * key_total / D,
    )


def solution(mesh):
    split = Mesh(mesh.devices.reshape(8, 4, 2, 2, 2), ("z", "x", "yh", "yl", "c"))
    tokens = ("z", "x", "yh", "yl")
    rows = P(("z", "x"), "c")
    heads = P("c", None, None)
    placed = (P(tokens, None), P(tokens, "c"), P(tokens, "c"), rows, rows, rows, rows)
    placed += (P(("z", "x"), None),) * 2 + (heads,) * 4
    whole = P(None, "c")
    return jax.shard_map(
        shards,
        mesh=split,
        in_specs=placed,
        out_specs=(rows, rows, rows, rows, whole, whole, rows, rows, heads, heads),
        check_vma=False,
    )
```
